32 devices in a mesh: ep: 4 (over y, x), tp: 8 (over z, core).
Axes of the slice: x: 2, y: 2, z: 4, core: 2. Of those that a mesh axis runs over, the one named last changes fastest.
Arguments:
- mixer_in: bfloat16 [8192, 2048], P(('ep', 'tp')), may hold values from -6 to 6
- pre_gain: float32 [2048], replicated, may hold values from 0.1 to 1.9
- glu_value: bfloat16 [2048, 1024], P(None, 'tp'), may hold values from -0.125 to 0.125
- glu_gate: bfloat16 [2048, 1024], P(None, 'tp'), may hold values from -0.125 to 0.125
- conv_kernel: float32 [31, 1024], replicated, may hold values from -1 to 1
- chan_gain: float32 [1024], replicated, may hold values from 0.1 to 1.9
- out_weight: bfloat16 [1024, 2048], P(None, 'tp'), may hold values from -0.1875 to 0.1875
- mix_gain: float32 [2048], replicated, may hold values from 0.1 to 1.9
- expert_in: bfloat16 [1024, 2048], P(('ep', 'tp')), may hold values from -6 to 6
- ffn_gain: float32 [2048], replicated, may hold values from 0.1 to 1.9
- routing: int32 [1024, 2], P(('ep', 'tp')), may hold values from 0 to 7, all different within a row; in each aligned block of 32 rows (0 to 31, 32 to 63, ...) at most 12 rows name the same one
- route_weight: float32 [1024, 2], P(('ep', 'tp')), may hold values from 0.1 to 1
- gate_proj: bfloat16 [8, 2048, 4096], P('ep', None, 'tp'), may hold values from -0.375 to 0.375
- up_proj: bfloat16 [8, 2048, 4096], P('ep', None, 'tp'), may hold values from -0.375 to 0.375
- down_proj: bfloat16 [8, 4096, 2048], P('ep', 'tp'), may hold values from -0.09375 to 0.09375
- expert_gain: float32 [2048], replicated, may hold values from 0.1 to 1.9
Outputs:
- mixed: bfloat16 [8192, 2048], P(('ep', 'tp'))
- routed: bfloat16 [1024, 2048], P(('ep', 'tp'))
The draws below stay inside these ranges and needn't reach their ends.
Inputs may be any that keep to these rules, and one draw needn't show every extreme that they name: `routing`: each row names 2 different experts; in each aligned block of 32 rows (the rows of one device) no expert is named more than 12 times.
All inputs are finite; a program needn't handle non-finite values.
Results may differ from the reference program's by a relative error of at most 0.02.
Values may be sent and summed in bfloat16 or wider, within the bound.
No kernel may reach another device: no remote copies, remote signals or barrier semaphores. Data moves between devices by JAX's collectives and lax.ppermute only.
A program may use at most 128 MiB of HBM per device.

```python
import math
import jax
import jax.numpy as jnp
import numpy as np
from jax import lax

D = 2048
C = 1024
FF = 4096
KERNEL = 31
TOPK = 2
SLICE = 32
EXPERTS = 8
CAPS = 12
TOKENS1 = 8192
TOKENS2 = 1024
N_EP = 4
N_TP = 8


def levels(own_key, extent, cuts, low, top_value):
    gain, own = 1.0, jax.random.fold_in(own_key, 6)
    for dim, parts in cuts:
        steps = jnp.exp(jax.random.uniform(jax.random.fold_in(own, dim), (parts,), jnp.float32, low / len(cuts), top_value / len(cuts)))
        gain = gain * jnp.repeat(steps, extent[dim] // parts).reshape([-1 if axis == dim else 1 for axis in range(len(extent))])
    return gain


def assign_block(stream_key, own, number, rows, amount, top, limit, skew):
    sequence = jax.random.permutation(stream_key, amount)
    crowded, ordinary = portions_of(amount, rows * top, limit, skew, True), portions_of(amount, rows * top, limit, skew, False)
    places = jnp.arange(amount)

    def named(lengths, offset_by):
        used = int((lengths > 0).sum())
        fixed = max(1, used // 4)
        passed = fixed + (places - fixed + offset_by * (used - fixed)) % max(1, amount - fixed)
        return jnp.zeros((amount,), jnp.int32).at[sequence[jnp.where(places < fixed, places, passed)]].set(jnp.asarray(lengths, jnp.int32))

    lengths = jnp.where(number % 4 == 0, named(crowded, number // 4), named(ordinary, number - number // 4 - 1))
    mixed = jax.random.permutation(jax.random.fold_in(own, 3), amount)
    giver, taker = mixed[0:amount // 2 * 2:2], mixed[1:amount // 2 * 2:2]
    room = jnp.minimum(lengths[giver] - 1, limit - lengths[taker]) // 2
    room = jnp.where((giver == sequence[0]) | (taker == sequence[0]) | (lengths[taker] == 0), 0, jnp.maximum(room, 0))
    passed = jax.random.randint(jax.random.fold_in(own, 4), (amount // 2,), 0, 1 << 20) % (room + 1)
    lengths = lengths.at[giver].add(-passed).at[taker].add(passed)
    items = jnp.searchsorted(jnp.cumsum(lengths), jnp.arange(rows * top), side="right").astype(jnp.int32)
    table = items.reshape(top, rows).T
    table = table[jax.random.permutation(jax.random.fold_in(own, 1), rows)]
    offset_by = jax.random.randint(jax.random.fold_in(own, 2), (rows, 1), 0, top)
    return jnp.take_along_axis(table, (jnp.arange(top)[None, :] + offset_by) % top, axis=1)


def portions_of(count, total, limit, skew, full):
    portions = [(1 << 20) // math.isqrt(grade ** skew) + 1 for grade in range(1, count + 1)]
    largest = limit if full else min(limit, max(-(-total // count), total * portions[0] // sum(portions)))
    least = 1 if total - largest >= count - 1 else 0
    counts, surplus = [largest] + [least] * (count - 1), total - largest - least * (count - 1)
    while surplus > 0:
        candidates = [i for i in range(1, count) if counts[i] < largest] or [i for i in range(1, count) if counts[i] < limit]
        whole, remaining = sum([portions[i] for i in candidates]), surplus
        for i in candidates:
            extra = min(limit - counts[i], max(1, remaining * portions[i] // whole), surplus)
            counts[i] = counts[i] + extra
            surplus = surplus - extra
    return np.array(counts)


def normal_values(own_key, dims, deviation, bound, pieces=(), kind=jnp.bfloat16):
    gain = levels(own_key, dims, pieces, -0.22, 0.18) if pieces else 1.0
    array = jax.random.normal(own_key, dims, jnp.float32) * deviation * gain
    return jnp.minimum(jnp.maximum(array, -bound), bound).astype(kind)


def setup_inputs(seed: int = 0) -> dict:
    splits = jax.random.split(jax.random.key(seed), 17)
    mixer_in = normal_values(splits[0], (TOKENS1, D), 1.0, 6.0, ((0, 32),))
    pre_gain = jnp.clip(1.0 + 0.18 * jax.random.normal(splits[1], (D,), jnp.float32), 0.1, 1.9)
    glu_value = normal_values(splits[2], (D, C), D ** -0.5, 0.125, ((1, 8),))
    glu_gate = normal_values(splits[3], (D, C), D ** -0.5, 0.125, ((1, 8),))
    conv_kernel = normal_values(splits[4], (KERNEL, C), KERNEL ** -0.5, 1.0, (), jnp.float32)
    chan_gain = jnp.clip(1.0 + 0.18 * jax.random.normal(splits[5], (C,), jnp.float32), 0.1, 1.9)
    out_weight = normal_values(splits[6], (C, D), C ** -0.5, 0.1875, ((1, 8),))
    mix_gain = jnp.clip(1.0 + 0.18 * jax.random.normal(splits[7], (D,), jnp.float32), 0.1, 1.9)
    expert_in = normal_values(splits[8], (TOKENS2, D), 1.0, 6.0, ((0, 32),))
    ffn_gain = jnp.clip(1.0 + 0.18 * jax.random.normal(splits[9], (D,), jnp.float32), 0.1, 1.9)
    routing_keys = jax.random.split(jax.random.fold_in(splits[10], 1), TOKENS2 // SLICE)
    routing_turns = jax.random.permutation(jax.random.fold_in(splits[10], 3), TOKENS2 // SLICE)
    routing = jax.vmap(lambda own, number: assign_block(jax.random.fold_in(splits[10], 2), own, number, SLICE, EXPERTS, TOPK, CAPS, 2))(routing_keys, routing_turns).reshape((TOKENS2, TOPK))
    route_weight = jnp.clip(0.1 + 0.9 * jax.random.uniform(splits[11], (TOKENS2, TOPK), jnp.float32) ** levels(splits[11], (TOKENS2, TOPK), ((0, 32),), -0.2, 0.2), 0.1, 1.0)
    gate_proj = normal_values(splits[12], (EXPERTS, D, FF), (D // 9) ** -0.5, 0.375, ((0, 4), (2, 8)))
    up_proj = normal_values(splits[13], (EXPERTS, D, FF), (D // 9) ** -0.5, 0.375, ((0, 4), (2, 8)))
    down_proj = normal_values(splits[14], (EXPERTS, FF, D), FF ** -0.5, 0.09375, ((0, 4), (1, 8)))
    expert_gain = jnp.clip(1.0 + 0.18 * jax.random.normal(splits[15], (D,), jnp.float32), 0.1, 1.9)
    return dict(mixer_in=mixer_in, pre_gain=pre_gain, glu_value=glu_value, glu_gate=glu_gate, conv_kernel=conv_kernel, chan_gain=chan_gain, out_weight=out_weight, mix_gain=mix_gain, expert_in=expert_in, ffn_gain=ffn_gain, routing=routing, route_weight=route_weight, gate_proj=gate_proj, up_proj=up_proj, down_proj=down_proj, expert_gain=expert_gain)


RMS_EPSILON = 1e-06
LAYER_EPSILON = 1e-05
CLAMP_LIMIT = 7.0
SWISH_ALPHA = 1.702

def rms_scale(values, gain_row):
    values = values.astype(jnp.float32)
    return values * lax.rsqrt(lax.optimization_barrier(jnp.mean(values * values, axis=-1, keepdims=True)) + RMS_EPSILON) * gain_row

def conv_mixer(mixer_in, pre_gain, glu_value, glu_gate, conv_kernel, chan_gain, out_weight, mix_gain):
    normed = rms_scale(mixer_in, pre_gain).astype(jnp.bfloat16)
    value_pre = jnp.dot(normed, glu_value, preferred_element_type=jnp.float32)
    gate_pre = jnp.dot(normed, glu_gate, preferred_element_type=jnp.float32)
    gated_rows = (value_pre * jax.nn.sigmoid(gate_pre)).astype(jnp.bfloat16)
    length = gated_rows.shape[0]
    padded = jnp.pad(gated_rows.astype(jnp.float32), ((KERNEL - 1, 0), (0, 0)))
    conv_sum = jnp.zeros((length, gated_rows.shape[1]), jnp.float32)
    for offset in range(KERNEL):
        conv_sum = conv_sum + conv_kernel[offset] * padded[offset:offset + length]
    row_mean = lax.optimization_barrier(jnp.mean(conv_sum, axis=-1, keepdims=True))
    centred = conv_sum - row_mean
    row_var = lax.optimization_barrier(jnp.mean(centred * centred, axis=-1, keepdims=True))
    activated = jax.nn.silu(centred * lax.rsqrt(row_var + LAYER_EPSILON) * chan_gain).astype(jnp.bfloat16)
    projected = jnp.dot(activated, out_weight, preferred_element_type=jnp.float32)
    return rms_scale(projected, mix_gain).astype(jnp.bfloat16)

def expert_layer(expert_in, ffn_gain, routing, route_weight, gate_proj, up_proj, down_proj, expert_gain):
    normed = rms_scale(expert_in, ffn_gain).astype(jnp.bfloat16)
    flat_route = routing.reshape(-1)
    flat_weight = route_weight.reshape(-1)
    capacity = N_EP * N_TP * CAPS
    hidden = gate_proj.shape[2] // N_TP

    def one_expert(running, expert):
        matches = flat_route == expert
        entry_index = jnp.nonzero(matches, size=capacity, fill_value=0)[0].astype(jnp.int32)
        live_count = jnp.sum(matches.astype(jnp.int32))
        live_slot = jnp.arange(capacity, dtype=jnp.int32) < live_count
        token_index = (entry_index // TOPK).astype(jnp.int32)
        row_block = normed[token_index]
        gate_pre = jnp.dot(row_block, gate_proj[expert], preferred_element_type=jnp.float32)
        up_pre = jnp.dot(row_block, up_proj[expert], preferred_element_type=jnp.float32)
        gate_pre = jnp.minimum(gate_pre, CLAMP_LIMIT)
        up_pre = jnp.clip(up_pre, -CLAMP_LIMIT, CLAMP_LIMIT)
        hidden_act = ((up_pre + 1.0) * gate_pre * jax.nn.sigmoid(SWISH_ALPHA * gate_pre)).astype(jnp.bfloat16)
        blocks = hidden_act.reshape(capacity, N_TP, hidden).astype(jnp.float32)
        down_block = down_proj[expert].reshape(N_TP, hidden, -1).astype(jnp.float32)
        partial_value = jnp.einsum('rnf,nfd->nrd', blocks, down_block).astype(jnp.bfloat16)
        expert_out = lax.optimization_barrier(jnp.sum(partial_value.astype(jnp.float32), axis=0)).astype(jnp.bfloat16)
        slot_weight = jnp.where(live_slot, flat_weight[entry_index], 0.0)
        running = running.at[token_index].add(slot_weight[:, None] * expert_out.astype(jnp.float32))
        return (running, None)
    start_sum = jnp.zeros(expert_in.shape, jnp.float32)
    combined, unused = lax.scan(one_expert, start_sum, jnp.arange(EXPERTS, dtype=jnp.int32))
    return rms_scale(combined, expert_gain).astype(jnp.bfloat16)

def reference(mixer_in, pre_gain, glu_value, glu_gate, conv_kernel, chan_gain, out_weight, mix_gain, expert_in, ffn_gain, routing, route_weight, gate_proj, up_proj, down_proj, expert_gain):
    mixed = conv_mixer(mixer_in, pre_gain, glu_value, glu_gate, conv_kernel, chan_gain, out_weight, mix_gain)
    routed = expert_layer(expert_in, ffn_gain, routing, route_weight, gate_proj, up_proj, down_proj, expert_gain)
    return (mixed, routed)
```

```python
import functools

import jax
import jax.numpy as jnp
from jax import lax
from jax.experimental import pallas as pl
from jax.experimental.pallas import tpu as pltpu
from jax.sharding import PartitionSpec as P

RMS_EPSILON = 1e-06
LAYER_EPSILON = 1e-05
CLAMP_LIMIT = 7.0
SWISH_ALPHA = 1.702


def passed_along(value, axis, steps):
    count = lax.axis_size(axis)
    initial, last = (max(0, -steps), min(count, count - steps))
    return lax.ppermute(value, axis, [(source, source + steps) for source in range(initial, last)])


def swapped(value, ep_bits, tp_bits):
    count_ep, count_tp = lax.axis_size("ep"), lax.axis_size("tp")
    pairs = [
        (e * count_tp + t, (e ^ ep_bits) * count_tp + (t ^ tp_bits))
        for e in range(count_ep)
        for t in range(count_tp)
    ]
    return lax.ppermute(value, ("ep", "tp"), pairs)


def rms_scale(values, gain_row):
    values = values.astype(jnp.float32)
    return (
        values
        * lax.rsqrt(jnp.mean(values * values, axis=-1, keepdims=True) + RMS_EPSILON)
        * gain_row
    )


def gathered_blocks(own):
    count_ep, count_z = lax.axis_size("ep"), lax.axis_size("tp") // 2
    quarter = own.shape[0] // count_ep
    mine = lax.dynamic_slice_in_dim(own, lax.axis_index("ep") * quarter, quarter, 0)
    column = jnp.stack([swapped(mine, 0, 2 * bits) for bits in range(1, count_z)])
    pieces = [column] + [swapped(column, bits, 0) for bits in range(1, count_ep)]
    other = (swapped(own, 0, 1), [swapped(piece, 0, 1) for piece in pieces])
    return (own, pieces), other


def block_products(rows_ref, places, own_ref, piece_refs, quarter, block, count_z):
    total = None
    for bits, piece in enumerate(piece_refs):
        if block == 0:
            columns, weight = bits, own_ref[bits * quarter : (bits + 1) * quarter, :]
        else:
            columns, weight = places[0] ^ bits, piece[block - 1]
        if len(rows_ref.shape) == 3:
            part = rows_ref[columns]
        else:
            part = rows_ref[:, pl.ds(pl.multiple_of(columns * quarter, quarter), quarter)]
        term = jnp.dot(part, weight, preferred_element_type=jnp.float32)
        total = term if total is None else total + term
    return total


def by_quarter(rows, count):
    length, depth = rows.shape
    if (depth // count) % 128 == 0:
        return rows
    return rows.reshape(length, count, depth // count).transpose(1, 0, 2)


def glu_body(count_z, count_ep, places, rows_ref, *refs):
    glu_ref = refs[-1]
    channels = glu_ref.shape[2]
    per_core = 1 + count_ep
    quarter = refs[0].shape[0] // count_ep
    for core in range(2):
        own_ref, piece_refs = refs[core * per_core], refs[core * per_core + 1 : (core + 1) * per_core]
        for block in range(count_z):
            pre = block_products(rows_ref, places, own_ref, piece_refs, quarter, block, count_z)
            out = pre[:, :channels] * jax.nn.sigmoid(pre[:, channels:])
            glu_ref[places[1] ^ (2 * block + core)] = out.astype(glu_ref.dtype)


def glu_rows(places, rows, weight_sets):
    count_ep, count_tp = lax.axis_size("ep"), lax.axis_size("tp")
    flat = []
    for own, pieces in weight_sets:
        flat += [own] + pieces
    channels = flat[0].shape[1] // 2
    length = rows.shape[0]
    depth = rows.shape[1]
    return pl.pallas_call(
        functools.partial(glu_body, count_tp // 2, count_ep),
        out_shape=jax.ShapeDtypeStruct((count_tp, length, channels), jnp.bfloat16),
        in_specs=[pl.BlockSpec(memory_space=pltpu.SMEM)]
        + [pl.BlockSpec(memory_space=pltpu.VMEM)] * (1 + len(flat)),
        out_specs=pl.BlockSpec(memory_space=pltpu.VMEM),
        cost_estimate=pl.CostEstimate(
            flops=4 * length * depth * channels * count_tp,
            bytes_accessed=4 * depth * channels * count_tp,
            transcendentals=length * channels * count_tp,
        ),
        name="glu",
    )(places, by_quarter(rows, count_ep), *flat)


def project_body(count_z, count_ep, places, rows_ref, gain_ref, *refs):
    out_ref, held = refs[-2], refs[-1]
    per_core = 1 + count_ep
    quarter = refs[0].shape[0] // count_ep
    width = refs[0].shape[1]
    squares = jnp.zeros((held.shape[0], 1), jnp.float32)
    for core in range(2):
        own_ref, piece_refs = refs[core * per_core], refs[core * per_core + 1 : (core + 1) * per_core]
        for block in range(count_z):
            pre = block_products(rows_ref, places, own_ref, piece_refs, quarter, block, count_z)
            squares = squares + jnp.sum(pre * pre, axis=-1, keepdims=True)
            start = pl.multiple_of((places[1] ^ (2 * block + core)) * width, width)
            held[:, pl.ds(start, width)] = pre
    scale = lax.rsqrt(squares / held.shape[1] + RMS_EPSILON)
    out_ref[...] = (held[...] * scale * gain_ref[...]).astype(out_ref.dtype)


def project_rows(places, rows, gain_row, weight_sets):
    count_ep, count_tp = lax.axis_size("ep"), lax.axis_size("tp")
    flat = []
    for own, pieces in weight_sets:
        flat += [own] + pieces
    length, depth = rows.shape
    width = flat[0].shape[1] * count_tp
    return pl.pallas_call(
        functools.partial(project_body, count_tp // 2, count_ep),
        out_shape=jax.ShapeDtypeStruct((length, width), jnp.bfloat16),
        in_specs=[pl.BlockSpec(memory_space=pltpu.SMEM)]
        + [pl.BlockSpec(memory_space=pltpu.VMEM)] * (2 + len(flat)),
        out_specs=pl.BlockSpec(memory_space=pltpu.VMEM),
        scratch_shapes=[pltpu.VMEM((length, width), jnp.float32)],
        cost_estimate=pl.CostEstimate(
            flops=2 * length * depth * width, bytes_accessed=2 * depth * width, transcendentals=0
        ),
        name="project",
    )(places, by_quarter(rows, count_ep), gain_row.reshape(1, -1), *flat)


def on_device(
    mixer_in,
    pre_gain,
    glu_value,
    glu_gate,
    conv_kernel,
    chan_gain,
    out_weight,
    mix_gain,
    expert_in,
    ffn_gain,
    routing,
    route_weight,
    gate_proj,
    up_proj,
    down_proj,
    expert_gain,
):
    count_ep, count_tp = lax.axis_size("ep"), lax.axis_size("tp")
    count_z = count_tp // 2
    ep_index, tp_index = lax.axis_index("ep"), lax.axis_index("tp")
    places = jnp.stack([ep_index, tp_index]).astype(jnp.int32)
    local_experts = gate_proj.shape[0]
    experts = local_experts * count_ep
    token_rows, top_count = routing.shape
    width = expert_in.shape[1]
    capacity = max(2, 3 * token_rows * top_count // (2 * experts))

    weight_high = route_weight.astype(jnp.bfloat16)
    weight_low = (route_weight - weight_high.astype(jnp.float32)).astype(jnp.bfloat16)
    extra = jnp.concatenate([routing.astype(jnp.bfloat16), weight_high, weight_low], axis=1)
    extra = jnp.pad(extra, ((0, 0), (0, 128 - extra.shape[1])))
    tokens = jnp.concatenate([expert_in, extra], axis=1)
    column = jnp.stack([tokens] + [swapped(tokens, 0, 2 * bits) for bits in range(1, count_z)])
    plane = [column] + [swapped(column, bits, 0) for bits in range(1, count_ep)]
    groups = plane + [swapped(block, 0, 1) for block in plane]
    every = jnp.stack(groups)
    group_rows = count_z * token_rows
    every = every.reshape(2 * count_ep, group_rows, width + 128)

    glu_sets = gathered_blocks(jnp.concatenate([glu_value, glu_gate], axis=1))
    out_sets = gathered_blocks(out_weight)

    slots = capacity * count_z
    extra = every[:, :, width:].astype(jnp.float32)
    named = extra[:, :, :top_count]
    shares = extra[:, :, top_count : 2 * top_count] + extra[:, :, 2 * top_count : 3 * top_count]
    local_ids = (ep_index * local_experts + jnp.arange(local_experts)).astype(jnp.float32)
    hits = named[:, :, None, :] == local_ids[None, None, :, None]
    hit = jnp.any(hits, axis=3)
    share = jnp.sum(jnp.where(hits, shares[:, :, None, :], 0.0), axis=3)
    below = jnp.tril(jnp.ones((group_rows, group_rows), jnp.float32), -1)
    rank = jnp.einsum("ab,gbe->gae", below, hit.astype(jnp.float32))
    chosen = (
        rank[:, :, :, None] == jnp.arange(slots, dtype=jnp.float32)[None, None, None, :]
    ) & hit[:, :, :, None]
    chosen = chosen.reshape(2 * count_ep, group_rows, local_experts * slots)
    pick = chosen.astype(jnp.bfloat16)
    slot_share = jnp.sum(
        jnp.where(
            chosen.reshape(2 * count_ep, group_rows, local_experts, slots),
            share[:, :, :, None],
            0.0,
        ),
        axis=1,
    )
    normed_exp = rms_scale(every[:, :, :width], ffn_gain).astype(jnp.bfloat16)
    rows = jnp.einsum("gts,gtd->gsd", pick, normed_exp, preferred_element_type=jnp.float32)
    rows = rows.astype(jnp.bfloat16).reshape(2 * count_ep, local_experts, slots, width)
    rows = rows.transpose(1, 0, 2, 3).reshape(local_experts, 2 * count_ep * slots, width)
    gate_pre = jnp.einsum("erd,edf->erf", rows, gate_proj, preferred_element_type=jnp.float32)
    up_pre = jnp.einsum("erd,edf->erf", rows, up_proj, preferred_element_type=jnp.float32)
    gate_pre = jnp.minimum(gate_pre, CLAMP_LIMIT)
    up_pre = jnp.clip(up_pre, -CLAMP_LIMIT, CLAMP_LIMIT)
    hidden = ((up_pre + 1.0) * gate_pre * jax.nn.sigmoid(SWISH_ALPHA * gate_pre)).astype(
        jnp.bfloat16
    )
    expert_out = jnp.einsum("erf,efd->erd", hidden, down_proj, preferred_element_type=jnp.float32)
    slot_share = slot_share.transpose(1, 0, 2).reshape(local_experts, 2 * count_ep * slots)
    weighted = (expert_out * slot_share[:, :, None]).astype(jnp.bfloat16)
    weighted = weighted.reshape(local_experts, 2 * count_ep, slots, width)
    weighted = weighted.transpose(1, 0, 2, 3).reshape(2 * count_ep, local_experts * slots, width)
    partial = jnp.einsum("gts,gsd->gtd", pick, weighted, preferred_element_type=jnp.float32)
    partial = partial.astype(jnp.bfloat16).reshape(2, count_ep, count_z, token_rows, width)

    def added(first, others):
        total = first.astype(jnp.float32)
        for other in others:
            total = total + other.astype(jnp.float32)
        return total

    chip = added(partial[0], [swapped(partial[1], 0, 1)]).astype(jnp.bfloat16)
    summed = added(chip[0], [swapped(chip[bits], bits, 0) for bits in range(1, count_ep)])
    summed = summed.astype(jnp.bfloat16)
    combined = added(
        summed[0], [swapped(summed[bits], 0, 2 * bits) for bits in range(1, count_z)]
    )
    routed = rms_scale(combined, expert_gain).astype(jnp.bfloat16)

    normed_mix = rms_scale(mixer_in, pre_gain).astype(jnp.bfloat16)
    glu_blocks = glu_rows(places, normed_mix, glu_sets)
    gated_rows = glu_blocks.transpose(1, 0, 2).reshape(mixer_in.shape[0], -1)
    kernel_width = conv_kernel.shape[0]
    length = gated_rows.shape[0]
    rim_rows = passed_along(gated_rows[length - (kernel_width - 1) :], ("ep", "tp"), 1)
    padded = jnp.concatenate([rim_rows, gated_rows], axis=0).astype(jnp.float32)
    conv_sum = jnp.zeros((length, gated_rows.shape[1]), jnp.float32)
    for offset in range(kernel_width):
        conv_sum = conv_sum + conv_kernel[offset] * padded[offset : offset + length]
    row_mean = jnp.mean(conv_sum, axis=-1, keepdims=True)
    centred = conv_sum - row_mean
    row_var = jnp.mean(centred * centred, axis=-1, keepdims=True)
    activated = jax.nn.silu(centred * lax.rsqrt(row_var + LAYER_EPSILON) * chan_gain).astype(
        jnp.bfloat16
    )
    mixed = project_rows(places, activated, mix_gain, out_sets)
    return (mixed, routed)


def solution(mesh):
    in_specs = (
        P(("ep", "tp"), None),
        P(),
        P(None, "tp"),
        P(None, "tp"),
        P(),
        P(),
        P(None, "tp"),
        P(),
        P(("ep", "tp"), None),
        P(),
        P(("ep", "tp"), None),
        P(("ep", "tp"), None),
        P("ep", None, "tp"),
        P("ep", None, "tp"),
        P("ep", "tp", None),
        P(),
    )
    out_specs = (P(("ep", "tp"), None), P(("ep", "tp"), None))
    return jax.shard_map(
        on_device, mesh=mesh, in_specs=in_specs, out_specs=out_specs, check_vma=False
    )
```

```python
import functools

import jax
import jax.numpy as jnp
from jax import lax
from jax.experimental import pallas as pl
from jax.experimental.pallas import tpu as pltpu
from jax.sharding import PartitionSpec as P


RMS_EPSILON = 1e-06
LAYER_EPSILON = 1e-05
CLAMP_LIMIT = 7.0
SWISH_ALPHA = 1.702
SPARE_VMEM = 6 * 1024 * 1024


def passed_along(value, axis, steps):
    count = lax.axis_size(axis)
    initial, last = (max(0, -steps), min(count, count - steps))
    return lax.ppermute(value, axis, [(source, source + steps) for source in range(initial, last)])


def swapped(value, ep_bits, tp_bits):
    count_ep, count_tp = lax.axis_size("ep"), lax.axis_size("tp")
    pairs = [
        (e * count_tp + t, (e ^ ep_bits) * count_tp + (t ^ tp_bits))
        for e in range(count_ep)
        for t in range(count_tp)
    ]
    return lax.ppermute(value, ("ep", "tp"), pairs)


def column_shared(value):
    return [swapped(value, 0, 2 * bits) for bits in range(1, lax.axis_size("tp") // 2)]


def plane_shared(value, axis):
    count_ep = lax.axis_size("ep")
    if count_ep != 4:
        return [[swapped(value, bits, 0)] for bits in range(1, count_ep)]
    half = value.shape[axis] // 2
    near = [swapped(value, 1, 0), swapped(value, 2, 0)]
    low = swapped(lax.slice_in_dim(near[0], 0, half, axis=axis), 2, 0)
    high = swapped(lax.slice_in_dim(near[1], half, 2 * half, axis=axis), 1, 0)
    return [[near[0]], [near[1]], [low, high]]


def rms_scale(values, gain_row):
    values = values.astype(jnp.float32)
    return (
        values
        * lax.rsqrt(jnp.mean(values * values, axis=-1, keepdims=True) + RMS_EPSILON)
        * gain_row
    )


def weights_body(places, value_ref, gate_ref, out_ref, glu_ref, glu_part_ref, out_part_ref):
    channels = value_ref.shape[1]
    glu_ref[:, :channels] = value_ref[...]
    glu_ref[:, channels:] = gate_ref[...]
    for full, part in ((value_ref, glu_part_ref), (gate_ref, glu_part_ref), (out_ref, out_part_ref)):
        depth = part.shape[0]
        start = pl.multiple_of(places[0] * depth, depth)
        rows = full[pl.ds(start, depth), :]
        if full is gate_ref:
            part[:, channels:] = rows
        else:
            part[:, : full.shape[1]] = rows


def gathered_blocks(own, mine):
    column = packed(column_shared(mine))
    pieces = [[column]] + plane_shared(column, 1)
    other = [[swapped(part, 0, 1) for part in parts] for parts in pieces]
    return (own, pieces), (swapped(own, 0, 1), other)


def flat_refs(weight_sets):
    return [
        part for own, pieces in weight_sets for part in [own] + [p for parts in pieces for p in parts]
    ]


def unflat_refs(refs, counts):
    sets, at = [], 0
    for _ in range(2):
        own, pieces = refs[at], []
        at += 1
        for count in counts:
            pieces.append(refs[at : at + count])
            at += count
        sets.append((own, pieces))
    return sets


def block_products(rows_ref, places, own_ref, pieces, quarter, block):
    total = None
    for bits, parts in enumerate(pieces):
        if block == 0:
            terms = [(0, quarter, own_ref[bits * quarter : (bits + 1) * quarter, :])]
        else:
            terms, at = [], 0
            for part in parts:
                terms.append((at, part.shape[1], part[block - 1]))
                at += part.shape[1]
        columns = bits if block == 0 else places[0] ^ bits
        for at, depth, weight in terms:
            if len(rows_ref.shape) == 3:
                rows = rows_ref[columns][:, at : at + depth]
            else:
                rows = rows_ref[:, pl.ds(pl.multiple_of(columns * quarter, quarter) + at, depth)]
            term = jnp.dot(rows, weight, preferred_element_type=jnp.float32)
            total = term if total is None else total + term
    return total


def by_quarter(rows, count):
    length, depth = rows.shape
    if (depth // count) % 128 == 0:
        return rows
    return rows.reshape(length, count, depth // count).transpose(1, 0, 2)


def glu_body(counts, places, rows_ref, *refs):
    glu_ref, rim_ref = refs[-2], refs[-1]
    channels = glu_ref.shape[2]
    quarter = refs[0].shape[0] // len(counts)
    for core, (own_ref, pieces) in enumerate(unflat_refs(refs, counts)):
        for block in range(glu_ref.shape[0] // 2):
            pre = block_products(rows_ref, places, own_ref, pieces, quarter, block)
            out = pre[:, :channels] * jax.nn.sigmoid(pre[:, channels:])
            out = out.astype(glu_ref.dtype)
            glu_ref[places[1] ^ (2 * block + core)] = out
            rim_ref[places[1] ^ (2 * block + core)] = out[-rim_ref.shape[1] :]


def glu_rows(places, rows, weight_sets, rim):
    count_ep, count_tp = lax.axis_size("ep"), lax.axis_size("tp")
    flat = flat_refs(weight_sets)
    counts = [len(parts) for parts in weight_sets[0][1]]
    channels = flat[0].shape[1] // 2
    length, depth = rows.shape
    return vmem_call(
        functools.partial(glu_body, counts),
        [shape_of((count_tp, length, channels)), shape_of((count_tp, rim, channels))],
        flops=4 * length * depth * channels * count_tp,
        moved=4 * depth * channels * count_tp,
    )(places, by_quarter(rows, count_ep), *flat)


def conv_body(taps, glu_ref, rim_ref, taps_ref, gain_ref, out_ref, held):
    blocks, length, channels = glu_ref.shape
    rim = rim_ref.shape[1]
    span = min(length, 128)
    for block in range(blocks):
        lanes = slice(block * channels, (block + 1) * channels)
        for first in range(0, length, span):
            if first == 0:
                above = rim_ref[block]
            else:
                above = glu_ref[block, first - rim : first, :]
            rows = jnp.concatenate([above, glu_ref[block, first : first + span, :]], axis=0)
            rows = rows.astype(jnp.float32)
            total = jnp.zeros((span, channels), jnp.float32)
            for turn in range(8):
                shifts = [s for s in range(rim - taps + 1, rim + 1) if s % 8 == turn]
                if not shifts:
                    continue
                moved = rows if turn == 0 else jnp.concatenate([rows[turn:], rows[:turn]], axis=0)
                for shift in shifts:
                    tap = shift - (rim - taps + 1)
                    base = shift - turn
                    total = total + taps_ref[tap : tap + 1, lanes] * moved[base : base + span]
            held[first : first + span, lanes] = total
    for first in range(0, length, 32):
        rows = held[first : first + 32, :]
        centred = rows - jnp.mean(rows, axis=-1, keepdims=True)
        spread = jnp.mean(centred * centred, axis=-1, keepdims=True)
        scaled = centred * lax.rsqrt(spread + LAYER_EPSILON) * gain_ref[...]
        out_ref[first : first + 32, :] = (scaled * jax.nn.sigmoid(scaled)).astype(out_ref.dtype)


def project_body(counts, places, rows_ref, gain_ref, *refs):
    out_ref, held = refs[-2], refs[-1]
    width = refs[0].shape[1]
    quarter = refs[0].shape[0] // len(counts)
    squares = jnp.zeros((held.shape[0], 1), jnp.float32)
    for core, (own_ref, pieces) in enumerate(unflat_refs(refs, counts)):
        for block in range(held.shape[1] // width // 2):
            pre = block_products(rows_ref, places, own_ref, pieces, quarter, block)
            squares = squares + jnp.sum(pre * pre, axis=-1, keepdims=True)
            start = pl.multiple_of((places[1] ^ (2 * block + core)) * width, width)
            held[:, pl.ds(start, width)] = pre
    scale = lax.rsqrt(squares / held.shape[1] + RMS_EPSILON)
    out_ref[...] = (held[...] * scale * gain_ref[...]).astype(out_ref.dtype)


def project_rows(places, rows, gain_row, weight_sets):
    count_ep, count_tp = lax.axis_size("ep"), lax.axis_size("tp")
    flat = flat_refs(weight_sets)
    counts = [len(parts) for parts in weight_sets[0][1]]
    length, depth = rows.shape
    width = flat[0].shape[1] * count_tp
    return pl.pallas_call(
        functools.partial(project_body, counts),
        out_shape=jax.ShapeDtypeStruct((length, width), jnp.bfloat16),
        in_specs=[pl.BlockSpec(memory_space=pltpu.SMEM)]
        + [pl.BlockSpec(memory_space=pltpu.VMEM)] * (2 + len(flat)),
        out_specs=pl.BlockSpec(memory_space=pltpu.VMEM),
        scratch_shapes=[pltpu.VMEM((length, width), jnp.float32)],
        cost_estimate=pl.CostEstimate(
            flops=2 * length * depth * width, bytes_accessed=2 * depth * width, transcendentals=0
        ),
        name="project",
    )(places, by_quarter(rows, count_ep), gain_row.reshape(1, -1), *flat)


def vmem_call(body, outs, scratch=(), flops=0, moved=0, smem=1):
    def call(*operands):
        arrays = list(operands[smem:]) + jax.tree.leaves(outs) + [held.inner_aval for held in scratch]
        held_bytes = sum(a.size * a.dtype.itemsize for a in arrays)
        return pl.pallas_call(
            body,
            out_shape=outs,
            in_specs=[pl.BlockSpec(memory_space=pltpu.SMEM)] * smem
            + [pl.BlockSpec(memory_space=pltpu.VMEM)] * (len(operands) - smem),
            out_specs=jax.tree.map(lambda _: pl.BlockSpec(memory_space=pltpu.VMEM), outs),
            scratch_shapes=list(scratch),
            compiler_params=pltpu.CompilerParams(vmem_limit_bytes=held_bytes + SPARE_VMEM),
            cost_estimate=pl.CostEstimate(
                flops=flops, bytes_accessed=moved, transcendentals=0
            ),
        )(*operands)

    return call


def shape_of(dims, kind=jnp.bfloat16):
    return jax.ShapeDtypeStruct(tuple(dims), kind)


def packed(parts):
    def body(*refs):
        for number, ref in enumerate(refs[:-1]):
            refs[-1][number] = ref[...]

    dims = (len(parts),) + parts[0].shape
    return vmem_call(body, shape_of(dims), flops=2 * parts[0].size, smem=0)(*parts)


def token_body(top_count, rows_ref, route_ref, share_ref, out_ref):
    _, width = rows_ref.shape
    out_ref[:, :width] = rows_ref[...]
    share = share_ref[...]
    high = share.astype(jnp.bfloat16).astype(jnp.float32)
    fields = jnp.concatenate([route_ref[...].astype(jnp.float32), high, share - high], axis=0)
    lanes = lax.broadcasted_iota(jnp.int32, (3 * top_count, 128), 1)
    places = lax.broadcasted_iota(jnp.int32, (3 * top_count, 128), 0)
    spread = jnp.where(lanes == places, 1.0, 0.0).astype(jnp.bfloat16)
    extra = lax.dot_general(
        fields.astype(jnp.bfloat16),
        spread,
        (((0,), (0,)), ((), ())),
        preferred_element_type=jnp.float32,
    )
    out_ref[:, width:] = extra.astype(out_ref.dtype)


def pick_body(layout, counts, places, gain_ref, *refs):
    experts, slots, top_count = layout
    parts, (rows_ref, chosen_ref, share_ref) = refs[:-3], refs[-3:]
    width = parts[0].shape[2] - 128
    gain = gain_ref[...]
    at = 0
    for group, count in enumerate(counts):
        block = jnp.concatenate(
            [
                part[number]
                for part in parts[at : at + count]
                for number in range(part.shape[0])
            ],
            axis=0,
        )
        at += count
        length = block.shape[0]
        below = (
            lax.broadcasted_iota(jnp.int32, (length, length), 0)
            > lax.broadcasted_iota(jnp.int32, (length, length), 1)
        ).astype(jnp.bfloat16)
        slot = lax.broadcasted_iota(jnp.int32, (length, slots), 1).astype(jnp.float32)
        lanes = lax.broadcasted_iota(jnp.int32, (length, 128), 1)
        named = block[:, width:].astype(jnp.float32)
        picks, sides = [], []
        for expert in range(experts):
            ident = (places[0] * experts + expert).astype(jnp.float32)
            hit = jnp.zeros((length, 1), jnp.float32)
            share = [jnp.zeros((length, 1), jnp.float32)] * 2
            for column in range(top_count):
                same = named[:, column : column + 1] == ident
                hit = jnp.where(same, 1.0, hit)
                for side in range(2):
                    lane = (side + 1) * top_count + column
                    share[side] = jnp.where(same, named[:, lane : lane + 1], share[side])
            mark = jnp.broadcast_to(hit, (length, 128)).astype(jnp.bfloat16)
            rank = jnp.dot(below, mark, preferred_element_type=jnp.float32)[:, 0:1]
            picks.append(jnp.where((slot == rank) & (hit > 0.0), 1.0, 0.0).astype(jnp.bfloat16))
            sides.append(jnp.where(lanes == 0, share[0], jnp.where(lanes == 1, share[1], 0.0)))
        pick = jnp.concatenate(picks, axis=1)
        chosen_ref[group] = pick
        taken = lax.dot_general(
            pick,
            block[:, :width],
            (((0,), (0,)), ((), ())),
            preferred_element_type=jnp.float32,
        )
        scale = lax.rsqrt(jnp.mean(taken * taken, axis=-1, keepdims=True) + RMS_EPSILON)
        taken = (taken * scale * gain).astype(jnp.bfloat16)
        for expert in range(experts):
            place = slice(group * slots, (group + 1) * slots)
            rows_ref[expert, place, :] = taken[expert * slots : (expert + 1) * slots]
            shares = lax.dot_general(
                picks[expert],
                sides[expert].astype(jnp.bfloat16),
                (((0,), (0,)), ((), ())),
                preferred_element_type=jnp.float32,
            )
            share_ref[expert, place, :] = jnp.broadcast_to(
                shares[:, 0:1] + shares[:, 1:2], (slots, 128)
            )


def picked(places, gain_row, groups, layout):
    experts, slots, _ = layout
    flat = [part for parts in groups for part in parts]
    length = sum(part.shape[0] * part.shape[1] for part in groups[0])
    width = flat[0].shape[2] - 128
    number = len(groups)
    outs = [
        shape_of((experts, number * slots, width)),
        shape_of((number, length, experts * slots)),
        shape_of((experts, number * slots, 128), jnp.float32),
    ]
    body = functools.partial(pick_body, layout, [len(parts) for parts in groups])
    return vmem_call(
        body, outs, flops=2 * number * length * 256 * width, moved=4 * number * length * width
    )(places, gain_row.reshape(1, -1), *flat)


def expert_body(sizes, gate_ref, up_ref, down_ref, *refs):
    count = len(sizes)
    ins, outs, rows = refs[:count], refs[count : 2 * count], refs[2 * count]
    at = 0
    for ref, size in zip(ins, sizes):
        rows[at : at + size] = ref[0]
        at += size
    inner = rows[...]
    gate_pre = jnp.dot(inner, gate_ref[0], preferred_element_type=jnp.float32)
    up_pre = jnp.dot(inner, up_ref[0], preferred_element_type=jnp.float32)
    gate_pre = jnp.minimum(gate_pre, CLAMP_LIMIT)
    up_pre = jnp.clip(up_pre, -CLAMP_LIMIT, CLAMP_LIMIT)
    hidden = ((up_pre + 1.0) * gate_pre * jax.nn.sigmoid(SWISH_ALPHA * gate_pre)).astype(
        jnp.bfloat16
    )
    outcome = jnp.dot(hidden, down_ref[0], preferred_element_type=jnp.float32).astype(jnp.bfloat16)
    at = 0
    for ref, size in zip(outs, sizes):
        ref[0] = outcome[at : at + size]
        at += size


def expert_rows(pieces, gate_proj, up_proj, down_proj):
    experts, width, hidden = gate_proj.shape
    sizes = [piece.shape[1] for piece in pieces]
    row_specs = [pl.BlockSpec((1, size, width), lambda j: (j, 0, 0)) for size in sizes]
    return pl.pallas_call(
        functools.partial(expert_body, sizes),
        grid=(experts,),
        out_shape=[shape_of(piece.shape) for piece in pieces],
        in_specs=[
            pl.BlockSpec((1, width, hidden), lambda j: (j, 0, 0)),
            pl.BlockSpec((1, width, hidden), lambda j: (j, 0, 0)),
            pl.BlockSpec((1, hidden, width), lambda j: (j, 0, 0)),
        ]
        + row_specs,
        out_specs=row_specs,
        scratch_shapes=[pltpu.VMEM((sum(sizes), width), jnp.bfloat16)],
        compiler_params=pltpu.CompilerParams(
            dimension_semantics=("arbitrary",),
            vmem_limit_bytes=12 * width * hidden + 10 * sum(sizes) * width + SPARE_VMEM
            + 20 * sum(sizes) * hidden,
        ),
        cost_estimate=pl.CostEstimate(
            flops=6 * experts * sum(sizes) * width * hidden,
            bytes_accessed=6 * experts * width * hidden,
            transcendentals=0,
        ),
        name="experts",
    )(gate_proj, up_proj, down_proj, *pieces)


def unpick_body(targets, counts, slots, *refs):
    outs = refs[4 * len(counts) :]
    group_at = 0
    for call, count in enumerate(counts):
        own_ref, other_ref, chosen_ref, share_ref = refs[4 * call : 4 * call + 4]
        for group in range(count):
            place = slice(group * slots, (group + 1) * slots)
            rows = jnp.concatenate(
                [
                    (
                        (own_ref[e, place, :].astype(jnp.float32) + other_ref[e, place, :].astype(jnp.float32))
                        * share_ref[e, place, 0:1]
                    ).astype(jnp.bfloat16)
                    for e in range(own_ref.shape[0])
                ],
                axis=0,
            )
            total = jnp.dot(chosen_ref[group], rows, preferred_element_type=jnp.float32)
            total = total.astype(jnp.bfloat16)
            size = total.shape[0] // len(targets[group_at])
            for part, (out, index) in enumerate(targets[group_at]):
                outs[out][index] = total[part * size : (part + 1) * size]
            group_at += 1


def modules(
    mixer_in,
    pre_gain,
    glu_value,
    glu_gate,
    conv_kernel,
    chan_gain,
    out_weight,
    mix_gain,
    expert_in,
    ffn_gain,
    routing,
    route_weight,
    gate_proj,
    up_proj,
    down_proj,
    expert_gain,
):
    count_ep, count_tp = lax.axis_size("ep"), lax.axis_size("tp")
    count_z = count_tp // 2
    ep_index, tp_index = lax.axis_index("ep"), lax.axis_index("tp")
    places = jnp.stack([ep_index, tp_index]).astype(jnp.int32)
    local_experts = gate_proj.shape[0]
    experts = local_experts * count_ep
    token_rows, top_count = routing.shape
    width = expert_in.shape[1]
    capacity = max(2, 3 * token_rows * top_count // (2 * experts))

    tokens = vmem_call(
        functools.partial(token_body, top_count),
        shape_of((token_rows, width + 128)),
        flops=1 << 18,
        smem=0,
    )(expert_in, routing.T, route_weight.T)
    column = packed([tokens] + column_shared(tokens))
    groups = [[column]] + plane_shared(column, 0)

    channels, columns = glu_value.shape[1], out_weight.shape[1]
    glu_own, glu_mine, out_mine = vmem_call(
        weights_body,
        [
            shape_of((width, 2 * channels)),
            shape_of((width // count_ep, 2 * channels)),
            shape_of((out_weight.shape[0] // count_ep, columns)),
        ],
        flops=1 << 20,
    )(places, glu_value, glu_gate, out_weight)
    glu_sets = gathered_blocks(glu_own, glu_mine)
    out_sets = gathered_blocks(out_weight, out_mine)

    slots = -(-capacity * count_z // 16) * 16
    layout = (local_experts, slots, top_count)
    near = picked(places, ffn_gain, groups[:1], layout)
    far = picked(places, ffn_gain, groups[1:], layout)
    pieces = [near[0], far[0]] + [swapped(near[0], 0, 1), swapped(far[0], 0, 1)]
    results = expert_rows(pieces, gate_proj, up_proj, down_proj)
    theirs = [swapped(results[2], 0, 1), swapped(results[3], 0, 1)]

    def added(*parts):
        total = parts[0].astype(jnp.float32)
        for part in parts[1:]:
            total = total + part.astype(jnp.float32)
        return total

    group_rows = count_z * token_rows
    if count_ep == 4:
        half = (2, group_rows // 2, width)
        outs = [shape_of((4,) + half[1:]), shape_of(half), shape_of(half)]
        targets = [[(0, 0), (0, 1)], [(1, 1), (0, 2)], [(0, 3), (2, 1)], [(1, 0), (2, 0)]]
    else:
        outs = [shape_of((count_ep, group_rows, width))]
        targets = [[(0, group)] for group in range(count_ep)]
    chip = vmem_call(
        functools.partial(unpick_body, targets, [1, count_ep - 1], slots),
        outs,
        flops=4 * count_ep * group_rows * 256 * width,
        smem=0,
    )(results[0], theirs[0], near[1], near[2], results[1], theirs[1], far[1], far[2])
    if count_ep == 4:
        first_x = swapped(chip[1], 1, 0)
        first_y = swapped(chip[2], 2, 0)
        passed_x = added(chip[0][2], first_y[0]).astype(jnp.bfloat16)
        passed_y = added(chip[0][3], first_x[0]).astype(jnp.bfloat16)
        last_x = swapped(passed_x, 1, 0)
        last_y = swapped(passed_y, 2, 0)
        summed = jnp.concatenate(
            [added(chip[0][0], first_x[1], last_y), added(chip[0][1], first_y[1], last_x)]
        )
    else:
        summed = added(
            chip[0][0], *[swapped(chip[0][bits], bits, 0) for bits in range(1, count_ep)]
        )
    summed = summed.astype(jnp.bfloat16).reshape(count_z, token_rows, width)
    combined = added(
        summed[0],
        *[swapped(summed[bits], 0, 2 * bits) for bits in range(1, count_z)],
    )
    routed = rms_scale(combined, expert_gain).astype(jnp.bfloat16)

    normed_mix = rms_scale(mixer_in, pre_gain).astype(jnp.bfloat16)
    taps = conv_kernel.shape[0]
    rim = -(-(taps - 1) // 16) * 16
    gated, last_rows = glu_rows(places, normed_mix, glu_sets, rim)
    rim_rows = passed_along(last_rows, ("ep", "tp"), 1)
    length = mixer_in.shape[0]
    activated = vmem_call(
        functools.partial(conv_body, taps),
        shape_of((length, conv_kernel.shape[1])),
        scratch=[pltpu.VMEM((length, conv_kernel.shape[1]), jnp.float32)],
        flops=1 << 32,
        smem=0,
    )(gated, rim_rows, conv_kernel, chan_gain.reshape(1, -1))
    mixed = project_rows(places, activated, mix_gain, out_sets)
    return (mixed, routed)


def solution(mesh):
    in_specs = (
        P(("ep", "tp"), None),
        P(),
        P(None, "tp"),
        P(None, "tp"),
        P(),
        P(),
        P(None, "tp"),
        P(),
        P(("ep", "tp"), None),
        P(),
        P(("ep", "tp"), None),
        P(("ep", "tp"), None),
        P("ep", None, "tp"),
        P("ep", None, "tp"),
        P("ep", "tp", None),
        P(),
    )
    out_specs = (P(("ep", "tp"), None), P(("ep", "tp"), None))
    return jax.shard_map(
        modules, mesh=mesh, in_specs=in_specs, out_specs=out_specs, check_vma=False
    )
```
